32 devices in a mesh: ep: 8 (over z, core), tp: 4 (over y, x).
Axes of the slice: x: 2, y: 2, z: 4, core: 2. Of those that a mesh axis runs over, the one named last changes fastest.
Arguments:
- attn_in: bfloat16 [4096, 2048], P('ep'), may hold values from -6 to 6
- mix_gain: float32 [2048], replicated, may hold values from 0.1 to 1.9
- query_weight: bfloat16 [2048, 1024], P(None, 'tp'), may hold values from -0.125 to 0.125
- key_weight: bfloat16 [2048, 1024], P(None, 'tp'), may hold values from -0.125 to 0.125
- value_weight: bfloat16 [2048, 1024], P(None, 'tp'), may hold values from -0.125 to 0.125
- query_gain: float32 [64], replicated, may hold values from 0.7 to 6
- key_gain: float32 [64], replicated, may hold values from 0.7 to 6
- log_cache: float32 [4096, 16], P('ep', 'tp'), as said below
- head_gain: float32 [1024], P('tp'), may hold values from 0.1 to 1.9
- out_weight: bfloat16 [1024, 2048], P(None, 'tp'), may hold values from -0.1875 to 0.1875
- moe_in: bfloat16 [1024, 2048], P('ep'), may hold values from -6 to 6
- moe_gain: float32 [2048], replicated, may hold values from 0.1 to 1.9
- routes: int32 [1024, 2], P('ep'), may hold values from 0 to 7, all different within a row; in each aligned block of 128 rows (0 to 127, 128 to 255, ...) at most 48 rows name the same one
- route_weight: float32 [1024, 2], P('ep'), may hold values from 0.25 to 1
- expert_gate: bfloat16 [8, 2048, 1024], P('ep', None, 'tp'), may hold values from -0.125 to 0.125
- expert_up: bfloat16 [8, 2048, 1024], P('ep', None, 'tp'), may hold values from -0.125 to 0.125
- expert_down: bfloat16 [8, 1024, 2048], P('ep', 'tp'), may hold values from -0.1875 to 0.1875
Outputs:
- mixer_out: bfloat16 [4096, 2048], P('ep', 'tp')
- moe_out: bfloat16 [1024, 2048], P('ep', 'tp')
The draws below stay inside these ranges and needn't reach their ends.
Inputs may be any that keep to these rules, and one draw needn't show every extreme that they name: `routes`: each row names 2 different experts; within the rows of one index of ep (aligned blocks of 128 rows) no expert is named by more than 48 rows. `log_cache`: never increasing along positions for each head.
All inputs are finite; a program needn't handle non-finite values.
Results may differ from the reference program's by a relative error of at most 0.015.
The reference program's roundings to bfloat16 on the way count: a program that leaves them out, or rounds other values in their place, can miss the bound.
Values may be sent and summed in bfloat16 or wider, within the bound.
A program may use at most 64 MiB of HBM per device.

```python
import math
import jax
import jax.numpy as jnp
import numpy as np
from jax import lax

D = 2048
HEADS = 16
HD = 64
FFE = 1024
TOPK = 2
TOK_DEV = 512
TOK_MOE = 128
TOKENS = 4096
TOKENS2 = 1024
EXPERTS = 8
CAP = 48
N_EP = 8


def draw_log_cache(key, part):
    first_key = jax.random.fold_in(key, 31)
    second_key = jax.random.fold_in(key, 32)
    third_key = jax.random.fold_in(key, 33)
    fast_heads = jax.random.uniform(first_key, (HEADS,), jnp.float32) < 0.5
    base_rate = jnp.where(fast_heads, 1.0 / 40.0, 1.5 / TOKENS)
    block_count = TOKENS // TOK_DEV
    block_factor = jnp.exp(jax.random.uniform(second_key, (block_count, 1, HEADS), jnp.float32, -0.7, 0.7))
    block_factor = jnp.broadcast_to(block_factor, (block_count, TOK_DEV, HEADS)).reshape(TOKENS, HEADS)
    rough_factor = jax.random.uniform(third_key, (TOKENS, HEADS), jnp.float32, 0.3, 1.7)
    return -jnp.cumsum(base_rate[None, :] * block_factor * rough_factor, axis=0)


def draw_query_gain(key, part):
    gain_key = jax.random.fold_in(key, 11)
    return jax.random.uniform(gain_key, (HD,), jnp.float32, 0.7, 1.3)


def draw_key_gain(key, part):
    gain_key = jax.random.fold_in(key, 12)
    return jax.random.uniform(gain_key, (HD,), jnp.float32, 0.7, 1.3)


def shard_levels(own_key, extent, pieces, smallest, top_value):
    loudness = 1.0
    for position, blocks in pieces:
        heights = jax.random.uniform(jax.random.fold_in(jax.random.fold_in(own_key, 6), position), (blocks,), jnp.float32, smallest / len(pieces), top_value / len(pieces))
        loudness = loudness * jnp.repeat(jnp.exp(heights), extent[position] // blocks).reshape((-1,) + (1,) * (len(extent) - 1 - position))
    return loudness


def assign_block(stream_key, own, number, rows, number_of, top, reach, slope):
    sequence = jax.random.permutation(stream_key, number_of)
    packed, usual = load_shares(number_of, rows * top, reach, slope, True), load_shares(number_of, rows * top, reach, slope, False)
    places = jnp.arange(number_of)

    def named(sizes, rotation):
        used = int((sizes > 0).sum())
        fixed = max(1, used // 4)
        shifted = fixed + (places - fixed + rotation * (used - fixed)) % max(1, number_of - fixed)
        return jnp.zeros((number_of,), jnp.int32).at[sequence[jnp.where(places < fixed, places, shifted)]].set(jnp.asarray(sizes, jnp.int32))

    sizes = jnp.where(number % 4 == 0, named(packed, number // 4), named(usual, number - number // 4 - 1))
    mixed = jax.random.permutation(jax.random.fold_in(own, 3), number_of)
    donor, sink = mixed[0:number_of // 2 * 2:2], mixed[1:number_of // 2 * 2:2]
    slack = jnp.minimum(sizes[donor] - 1, reach - sizes[sink]) // 2
    slack = jnp.where((donor == sequence[0]) | (sink == sequence[0]) | (sizes[sink] == 0), 0, jnp.maximum(slack, 0))
    shifted = jax.random.randint(jax.random.fold_in(own, 4), (number_of // 2,), 0, 1 << 20) % (slack + 1)
    sizes = sizes.at[donor].add(-shifted).at[sink].add(shifted)
    items = jnp.searchsorted(jnp.cumsum(sizes), jnp.arange(rows * top), side="right").astype(jnp.int32)
    grid = items.reshape(top, rows).T
    grid = grid[jax.random.permutation(jax.random.fold_in(own, 1), rows)]
    rotation = jax.random.randint(jax.random.fold_in(own, 2), (rows, 1), 0, top)
    return jnp.take_along_axis(grid, (jnp.arange(top)[None, :] + rotation) % top, axis=1)


def load_shares(count, total, limit, lean, full):
    loads = [(1 << 20) // math.isqrt(grade ** lean) + 1 for grade in range(1, count + 1)]
    largest = limit if full else min(limit, max(-(-total // count), total * loads[0] // sum(loads)))
    least = 1 if total - largest >= count - 1 else 0
    counts, spare = [largest] + [least] * (count - 1), total - largest - least * (count - 1)
    while spare > 0:
        candidates = [i for i in range(1, count) if counts[i] < largest] or [i for i in range(1, count) if counts[i] < limit]
        pool, left = sum([loads[i] for i in candidates]), spare
        for i in candidates:
            more = min(limit - counts[i], max(1, left * loads[i] // pool), spare)
            counts[i] = counts[i] + more
            spare = spare - more
    return np.array(counts)


def gaussian(key, extent, deviation, most, pieces=(), kind=jnp.bfloat16):
    entries = deviation * jax.random.normal(key, extent, jnp.float32)
    if pieces:
        entries = entries * shard_levels(key, extent, pieces, -0.22, 0.18)
    return jnp.clip(entries, -most, most).astype(kind)


def setup_inputs(seed: int = 0) -> dict:
    arg_keys = jax.random.split(jax.random.key(seed), 18)
    attn_in = gaussian(arg_keys[0], (TOKENS, D), 1.0, 6.0, ((0, 8),))
    mix_gain = jnp.clip(1.0 + 0.18 * jax.random.normal(arg_keys[1], (D,), jnp.float32), 0.1, 1.9)
    query_weight = gaussian(arg_keys[2], (D, HEADS * HD), D ** -0.5, 0.125, ((1, 4),))
    key_weight = gaussian(arg_keys[3], (D, HEADS * HD), D ** -0.5, 0.125, ((1, 4),))
    value_weight = gaussian(arg_keys[4], (D, HEADS * HD), D ** -0.5, 0.125, ((1, 4),))
    query_gain = draw_query_gain(jax.random.fold_in(arg_keys[17], 71), 0)
    key_gain = draw_key_gain(jax.random.fold_in(arg_keys[17], 71), 0)
    log_cache = draw_log_cache(jax.random.fold_in(arg_keys[17], 71), 0)
    head_gain = jnp.clip(1.0 + 0.18 * jax.random.normal(arg_keys[8], (HEADS * HD,), jnp.float32), 0.1, 1.9)
    out_weight = gaussian(arg_keys[9], (HEADS * HD, D), (HEADS * HD) ** -0.5, 0.1875, ((1, 4),))
    moe_in = gaussian(arg_keys[10], (TOKENS2, D), 1.0, 6.0, ((0, 8),))
    moe_gain = jnp.clip(1.0 + 0.18 * jax.random.normal(arg_keys[11], (D,), jnp.float32), 0.1, 1.9)
    routes_keys = jax.random.split(jax.random.fold_in(arg_keys[12], 1), TOKENS2 // TOK_MOE)
    routes_turns = jax.random.permutation(jax.random.fold_in(arg_keys[12], 3), TOKENS2 // TOK_MOE)
    routes = jax.vmap(lambda own, number: assign_block(jax.random.fold_in(arg_keys[12], 2), own, number, TOK_MOE, EXPERTS, TOPK, CAP, 1))(routes_keys, routes_turns).reshape((TOKENS2, TOPK))
    route_weight = jnp.clip(jnp.exp(math.log(1.0) - 1.3862944 * jax.random.uniform(arg_keys[13], (TOKENS2, TOPK), jnp.float32) ** shard_levels(arg_keys[13], (TOKENS2, TOPK), ((0, 8),), -0.2, 0.2)), 0.25, 1.0)
    expert_gate = gaussian(arg_keys[14], (EXPERTS, D, FFE), D ** -0.5, 0.125, ((0, 8), (2, 4)))
    expert_up = gaussian(arg_keys[15], (EXPERTS, D, FFE), D ** -0.5, 0.125, ((0, 8), (2, 4)))
    expert_down = gaussian(arg_keys[16], (EXPERTS, FFE, D), FFE ** -0.5, 0.1875, ((0, 8), (1, 4)))
    return {"attn_in": attn_in, "mix_gain": mix_gain, "query_weight": query_weight, "key_weight": key_weight, "value_weight": value_weight, "query_gain": query_gain, "key_gain": key_gain, "log_cache": log_cache, "head_gain": head_gain, "out_weight": out_weight, "moe_in": moe_in, "moe_gain": moe_gain, "routes": routes, "route_weight": route_weight, "expert_gate": expert_gate, "expert_up": expert_up, "expert_down": expert_down}


epsilon = 1e-06

def row_norm(inputs, gain_vec):
    floats = inputs.astype(jnp.float32)
    scaled = floats * lax.rsqrt(lax.optimization_barrier(jnp.mean(floats * floats, axis=-1, keepdims=True)) + epsilon)
    return scaled * gain_vec.astype(jnp.float32)

def reference(attn_in, mix_gain, query_weight, key_weight, value_weight, query_gain, key_gain, log_cache, head_gain, out_weight, moe_in, moe_gain, routes, route_weight, expert_gate, expert_up, expert_down):
    seq_len = attn_in.shape[0]
    normed = row_norm(attn_in, mix_gain).astype(jnp.bfloat16)

    def project(weight):
        return jnp.dot(normed, weight, preferred_element_type=jnp.float32).reshape(seq_len, HEADS, HD)
    queries = row_norm(project(query_weight), query_gain).astype(jnp.bfloat16)
    key_rows = row_norm(project(key_weight), key_gain).astype(jnp.bfloat16)
    value_rows = project(value_weight).astype(jnp.bfloat16)
    block_len = math.gcd(seq_len, 512)
    block_count = seq_len // block_len
    positions = jnp.arange(seq_len, dtype=jnp.int32)
    score_scale = HD ** (-0.5)

    def one_block(flat_index):
        head_index = flat_index // block_count
        block_begin = flat_index % block_count * block_len
        head_queries = lax.dynamic_index_in_dim(queries, head_index, 1, False)
        query_block = lax.dynamic_slice_in_dim(head_queries, block_begin, block_len, 0)
        head_keys = lax.dynamic_index_in_dim(key_rows, head_index, 1, False)
        head_values = lax.dynamic_index_in_dim(value_rows, head_index, 1, False)
        head_gates = lax.dynamic_index_in_dim(log_cache, head_index, 1, False)
        query_gates = lax.dynamic_slice_in_dim(head_gates, block_begin, block_len, 0)
        scores = jnp.dot(query_block, head_keys.T, preferred_element_type=jnp.float32) * score_scale
        scores = scores + query_gates[:, None] - head_gates[None, :]
        query_pos = block_begin + jnp.arange(block_len, dtype=jnp.int32)
        causal = positions[None, :] <= query_pos[:, None]
        scores = jnp.where(causal, scores, -jnp.inf)
        row_max = lax.optimization_barrier(jnp.max(scores, axis=1, keepdims=True))
        expo_scores = jnp.exp(scores - row_max)
        denominator = lax.optimization_barrier(jnp.sum(expo_scores, axis=1, keepdims=True))
        mixed_rows = jnp.dot(expo_scores.astype(jnp.bfloat16), head_values, preferred_element_type=jnp.float32)
        return mixed_rows / denominator
    blocks = lax.map(one_block, jnp.arange(HEADS * block_count, dtype=jnp.int32))
    attended = jnp.transpose(blocks.reshape(HEADS, seq_len, HD), (1, 0, 2))
    head_out = row_norm(attended, head_gain.reshape(HEADS, HD)).astype(jnp.bfloat16).reshape(seq_len, HEADS * HD)
    mixer_out = jnp.dot(head_out, out_weight, preferred_element_type=jnp.float32).astype(jnp.bfloat16)
    moe_normed = row_norm(moe_in, moe_gain).astype(jnp.bfloat16)
    flat_routes = routes.reshape(-1)
    slot_total = N_EP * CAP

    def one_expert(expert):
        chosen = flat_routes == expert
        picked = jnp.nonzero(chosen, size=slot_total, fill_value=0)[0].astype(jnp.int32)
        alive_mask = (jnp.arange(slot_total, dtype=jnp.int32) < jnp.sum(chosen.astype(jnp.int32))).astype(jnp.float32)
        token_rows = moe_normed[picked // TOPK]
        gate_w = lax.dynamic_index_in_dim(expert_gate, expert, 0, False)
        up_w = lax.dynamic_index_in_dim(expert_up, expert, 0, False)
        down_w = lax.dynamic_index_in_dim(expert_down, expert, 0, False)
        gate_sum = jnp.dot(token_rows, gate_w, preferred_element_type=jnp.float32)
        up_sum = jnp.dot(token_rows, up_w, preferred_element_type=jnp.float32)
        hidden = (jax.nn.silu(gate_sum) * up_sum).astype(jnp.bfloat16)
        expert_rows = jnp.dot(hidden, down_w, preferred_element_type=jnp.float32).astype(jnp.bfloat16)
        return (picked, alive_mask, expert_rows)
    picked, alive_mask, expert_rows = lax.map(one_expert, jnp.arange(EXPERTS, dtype=jnp.int32))
    flat_weight = route_weight.reshape(-1)
    scaled_rows = expert_rows.astype(jnp.float32) * (flat_weight[picked] * alive_mask)[:, :, None]
    token_index = (picked // TOPK).reshape(-1)
    moe_sum = jnp.zeros((flat_routes.shape[0] // TOPK, D), jnp.float32).at[token_index].add(scaled_rows.reshape(-1, D))
    moe_out = moe_sum.astype(jnp.bfloat16)
    return (mixer_out, moe_out)
```

```python
import functools

import jax
import jax.numpy as jnp
from jax import lax
from jax.experimental import pallas as pl
from jax.experimental.pallas import tpu as pltpu
from jax.sharding import PartitionSpec as P

HD = 64
LANES = 128
epsilon = 1e-06
BF = jnp.bfloat16
F32 = jnp.float32


def row_norm(inputs, gain_vec):
    floats = inputs.astype(F32)
    scaled = floats * lax.rsqrt(jnp.mean(floats * floats, axis=-1, keepdims=True) + epsilon)
    return scaled * gain_vec


def split3(x):
    hi = lax.reduce_precision(x, 8, 7)
    rest = x - hi
    mid = lax.reduce_precision(rest, 8, 7)
    return hi.astype(BF), mid.astype(BF), (rest - mid).astype(BF)


def attend_kernel(heads, q_ref, k_ref, v_ref, aug_ref, gain_ref, o_ref, qz, m_s, l_s, acc):
    me = lax.axis_index("ep")
    tok = q_ref.shape[1]
    row = lax.broadcasted_iota(jnp.int32, (LANES, tok), 0)
    zeros = jnp.zeros((HD, tok), BF)
    for h in range(heads):
        q_h = q_ref[h * HD:(h + 1) * HD, :]
        parts = [q_h, zeros] if h % 2 == 0 else [zeros, q_h]
        pick = jnp.where((row >= 3 * h) & (row < 3 * h + 3), -1.0, 0.0).astype(BF)
        qz[h] = jnp.concatenate(parts + [pick], axis=0)

    def step(block, first, masked):
        aug = aug_ref[block]
        for h in range(heads):
            p = h // 2
            keys = jnp.concatenate([k_ref[block, :, p * LANES:(p + 1) * LANES], aug], axis=1)
            s = jnp.dot(keys, qz[h], preferred_element_type=F32)
            if masked:
                kpos = lax.broadcasted_iota(jnp.int32, s.shape, 0)
                qpos = lax.broadcasted_iota(jnp.int32, s.shape, 1)
                s = jnp.where(kpos <= qpos, s, -1e30)
            top = jnp.max(s, axis=0, keepdims=True)
            if first:
                new = top
            else:
                new = jnp.maximum(m_s[h], top)
            e = jnp.exp(s - new)
            total = jnp.sum(e, axis=0, keepdims=True)
            o = jnp.dot(v_ref[block, h * HD:(h + 1) * HD, :], e.astype(BF), preferred_element_type=F32)
            if first:
                l_s[h] = total
                acc[h] = o
            else:
                fix = jnp.exp(m_s[h] - new)
                l_s[h] = l_s[h] * fix + total
                acc[h] = acc[h] * fix + o
            m_s[h] = new

    step(me, True, True)

    @pl.loop(0, me)
    def _(i):
        step(i, False, False)

    for h in range(heads):
        a = acc[h] / l_s[h]
        a = a * lax.rsqrt(jnp.mean(a * a, axis=0, keepdims=True) + epsilon)
        o_ref[h * HD:(h + 1) * HD, :] = (a * gain_ref[h * HD:(h + 1) * HD, :]).astype(BF)


def attend(q_t, k_all, v_all, aug, gain):
    feats, tok = q_t.shape
    heads = feats // HD
    vm = pl.BlockSpec(memory_space=pltpu.VMEM)
    blocks = k_all.shape[0]
    scores = heads * blocks * tok * tok
    return pl.pallas_call(
        functools.partial(attend_kernel, heads),
        out_shape=jax.ShapeDtypeStruct((feats, tok), BF),
        in_specs=[vm] * 5,
        out_specs=vm,
        scratch_shapes=[
            pltpu.VMEM((heads, 2 * LANES, tok), BF),
            pltpu.VMEM((heads, 1, tok), F32),
            pltpu.VMEM((heads, 1, tok), F32),
            pltpu.VMEM((heads, HD, tok), F32),
        ],
        compiler_params=pltpu.CompilerParams(vmem_limit_bytes=56 * 1024 * 1024),
        cost_estimate=pl.CostEstimate(flops=scores * 512, bytes_accessed=2**23, transcendentals=scores),
    )(q_t, k_all, v_all, aug, gain)


def body(
    attn_in,
    mix_gain,
    query_weight,
    key_weight,
    value_weight,
    query_gain,
    key_gain,
    log_cache,
    head_gain,
    out_weight,
    moe_in,
    moe_gain,
    routes,
    route_weight,
    expert_gate,
    expert_up,
    expert_down,
):
    tok_rows = attn_in.shape[0]
    feats = query_weight.shape[1]
    local_heads = feats // HD
    normed = row_norm(attn_in, mix_gain).astype(BF)

    def project(weight):
        return lax.dot_general(weight, normed, (((0,), (1,)), ((), ())), preferred_element_type=F32)

    def head_norm(x, gain):
        x = x.reshape(local_heads, HD, tok_rows)
        x = x * lax.rsqrt(jnp.mean(x * x, axis=1, keepdims=True) + epsilon)
        return (x * gain[None, :, None]).astype(BF).reshape(feats, tok_rows)

    k_rows = jnp.transpose(head_norm(project(key_weight), key_gain))
    if feats % LANES:
        k_rows = jnp.pad(k_rows, ((0, 0), (0, LANES - feats % LANES)))
    v_t = project(value_weight).astype(BF)
    k_all = lax.all_gather(k_rows, "ep")
    v_all = lax.all_gather(v_t, "ep")
    q_t = head_norm(project(query_weight), query_gain) * jnp.asarray(HD ** -0.5, BF)
    gates = lax.all_gather(log_cache, "ep")
    hi, mid, low = split3(gates)
    aug = jnp.stack([hi, mid, low], axis=-1).reshape(gates.shape[0], tok_rows, 3 * local_heads)
    aug = jnp.pad(aug, ((0, 0), (0, 0), (0, LANES - 3 * local_heads)))
    head_t = attend(q_t, k_all, v_all, aug, head_gain[:, None])
    mixer_out = lax.dot_general(
        lax.all_gather(head_t, "tp", axis=0, tiled=True),
        out_weight,
        (((0,), (0,)), ((), ())),
        preferred_element_type=F32,
    ).astype(BF)

    moe_rows = moe_in.shape[0]
    top_count = routes.shape[1]
    local_experts = expert_gate.shape[0]
    senders = lax.axis_size("ep")
    expert_count = local_experts * senders
    capacity = 3 * moe_rows * top_count // (2 * expert_count)
    model_width = moe_in.shape[1]
    moe_normed = row_norm(moe_in, moe_gain).astype(BF)
    flat_routes = routes.reshape(-1)
    one_hot = (flat_routes[:, None] == jnp.arange(expert_count, dtype=jnp.int32)[None, :]).astype(
        jnp.int32
    )
    order_in = jnp.sum(jnp.cumsum(one_hot, axis=0) * one_hot, axis=1) - 1
    slot_index = flat_routes * capacity + order_in
    slots = jnp.arange(expert_count * capacity, dtype=jnp.int32)
    hit = (slots[:, None, None] == slot_index.reshape(1, moe_rows, top_count)).any(axis=2)
    share_width = model_width // lax.axis_size("tp")
    my_share = lax.dynamic_slice_in_dim(moe_normed, lax.axis_index("tp") * share_width, share_width, 1)
    share_part = (
        jnp.dot(hit.astype(BF), my_share, preferred_element_type=F32)
        .astype(BF)
        .reshape(expert_count, capacity, share_width)
    )
    arrived = lax.all_to_all(share_part, "ep", split_axis=0, concat_axis=0, tiled=True)
    piece_now = lax.all_gather(arrived, "tp", axis=2, tiled=True)
    piece_cols = piece_now.shape[2]
    piece_rows = piece_now.reshape(senders, local_experts, capacity, piece_cols)
    gate_next = jnp.einsum("sjcd,jdf->sjcf", piece_rows, expert_gate, preferred_element_type=F32)
    up_next = jnp.einsum("sjcd,jdf->sjcf", piece_rows, expert_up, preferred_element_type=F32)
    hidden = (jax.nn.silu(gate_next) * up_next).astype(BF)
    partial_value = jnp.einsum("sjcf,jfd->sjcd", hidden, expert_down, preferred_element_type=F32)
    summed = lax.psum_scatter(partial_value.astype(BF), "tp", scatter_dimension=3, tiled=True)
    out_cols = summed.shape[3]
    returned = lax.all_to_all(
        summed.reshape(expert_count, capacity, out_cols),
        "ep",
        split_axis=0,
        concat_axis=0,
        tiled=True,
    )
    flat = returned.reshape(expert_count * capacity, out_cols)
    pick = (slot_index[:, None] == slots[None, :]).astype(BF)
    picked = jnp.dot(pick, flat, preferred_element_type=F32)
    weighted_rows = picked * route_weight.reshape(-1)[:, None]
    moe_out = jnp.sum(weighted_rows.reshape(moe_rows, top_count, out_cols), axis=1).astype(BF)
    return (mixer_out, moe_out)


def solution(mesh):
    in_specs = (
        P("ep", None),
        P(),
        P(None, "tp"),
        P(None, "tp"),
        P(None, "tp"),
        P(),
        P(),
        P("ep", "tp"),
        P("tp"),
        P(None, "tp"),
        P("ep", None),
        P(),
        P("ep", None),
        P("ep", None),
        P("ep", None, "tp"),
        P("ep", None, "tp"),
        P("ep", "tp", None),
    )
    out_specs = (P("ep", "tp"), P("ep", "tp"))
    return jax.shard_map(body, mesh=mesh, in_specs=in_specs, out_specs=out_specs, check_vma=False)
```

```python
import functools

import jax
import jax.numpy as jnp
from jax import lax
from jax.experimental import pallas as pl
from jax.experimental.pallas import tpu as pltpu
from jax.sharding import PartitionSpec as P

HD = 64
LANES = 128
epsilon = 1e-06
BF = jnp.bfloat16
F32 = jnp.float32


def row_norm(inputs, gain_vec):
    floats = inputs.astype(F32)
    scaled = floats * lax.rsqrt(jnp.mean(floats * floats, axis=-1, keepdims=True) + epsilon)
    return scaled * gain_vec


def attend_kernel(
    heads, count, q_ref, k_ref, v_ref, g_ref, gain_ref, o_ref,
    k_all, v_all, g_all, qz, m_s, l_s, acc, send_sem, recv_sem,
):
    me = lax.axis_index("ep")
    chips = count // 2
    z = me // 2
    c = me % 2
    other = 2 * z + 1 - c
    above = 2 * lax.rem(z + 1, chips) + c
    below = 2 * lax.rem(z + chips - 1, chips) + c
    tok = q_ref.shape[1]
    rows8 = g_ref.shape[0]
    own = (k_ref, v_ref, g_ref)
    slots = (k_all, v_all, g_all)

    barrier = pltpu.get_barrier_semaphore()
    for peer in (other, above, below):
        pl.semaphore_signal(barrier, inc=1, device_id={"ep": peer}, device_id_type=pl.DeviceIdType.MESH)
    pl.semaphore_wait(barrier, 3)

    def copies(refs, src, way, dist, target):
        return [
            pltpu.make_async_remote_copy(
                src_ref=refs[i],
                dst_ref=slots[i].at[src],
                send_sem=send_sem.at[i, way, dist],
                recv_sem=recv_sem.at[i, src],
                device_id={"ep": target},
                device_id_type=pl.DeviceIdType.MESH,
            )
            for i in range(3)
        ]

    def held(src):
        return [s.at[src] for s in slots]

    has_up = z + 1 < chips

    @pl.when(has_up)
    def _():
        for d in copies(own, me, 0, 0, above):
            d.start()

    @pl.when(c == 0)
    def _():
        for d in copies(own, me, 1, 0, other):
            d.start()

    row = lax.broadcasted_iota(jnp.int32, (LANES, tok), 0)
    zeros = jnp.zeros((HD, tok), BF)
    for h in range(heads):
        q_h = q_ref[h * HD:(h + 1) * HD, :]
        parts = [q_h, zeros] if h % 2 == 0 else [zeros, q_h]
        hit = (row == h) | (row == rows8 + h) | (row == 2 * rows8 + h)
        pick = jnp.where(hit, -1.0, 0.0).astype(BF)
        qz[h] = jnp.concatenate(parts + [pick], axis=0)

    def step(k_blk, v_blk, g_blk, first=False):
        g = g_blk[...]
        hi = g.astype(BF).astype(F32)
        rest = g - hi
        mid = rest.astype(BF).astype(F32)
        pad = jnp.zeros((LANES - 3 * rows8, tok), F32)
        aug = jnp.concatenate([hi, mid, rest - mid, pad], axis=0).T.astype(BF)
        for h in range(heads):
            p = h // 2
            keys = jnp.concatenate([k_blk[:, p * LANES:(p + 1) * LANES], aug], axis=1)
            s = jnp.dot(keys, qz[h], preferred_element_type=F32)
            if first:
                kpos = lax.broadcasted_iota(jnp.int32, s.shape, 0)
                qpos = lax.broadcasted_iota(jnp.int32, s.shape, 1)
                s = jnp.where(kpos <= qpos, s, -1e30)
            top = jnp.max(s, axis=0, keepdims=True)
            new = top if first else jnp.maximum(m_s[h], top)
            e = jnp.exp(s - new)
            total = jnp.sum(e, axis=0, keepdims=True)
            o = jnp.dot(v_blk[h * HD:(h + 1) * HD, :], e.astype(BF), preferred_element_type=F32)
            if first:
                l_s[h] = total
                acc[h] = o
            else:
                fix = jnp.exp(m_s[h] - new)
                l_s[h] = l_s[h] * fix + total
                acc[h] = acc[h] * fix + o
            m_s[h] = new

    step(*own, first=True)

    def take(src):
        for d in copies(held(src), src, 0, 0, other):
            d.wait_recv()

    @pl.when(c == 1)
    def _():
        take(other)
        step(*held(other))

    @pl.loop(1, z + 1)
    def _(dist):
        src = 2 * (z - dist) + c
        take(src)

        @pl.when(has_up)
        def _():
            for d in copies(held(src), src, 0, dist, above):
                d.start()

        for d in copies(held(src), src, 1, dist, other):
            d.start()
        step(*held(src))
        src2 = 2 * (z - dist) + 1 - c
        take(src2)
        step(*held(src2))

    for h in range(heads):
        a = acc[h] / l_s[h]
        a = a * lax.rsqrt(jnp.mean(a * a, axis=0, keepdims=True) + epsilon)
        o_ref[h * HD:(h + 1) * HD, :] = (a * gain_ref[h * HD:(h + 1) * HD, :]).astype(BF)

    @pl.when(has_up)
    def _():
        for d in copies(own, me, 0, 0, above):
            d.wait_send()

    @pl.when(c == 0)
    def _():
        for d in copies(own, me, 1, 0, other):
            d.wait_send()

    @pl.loop(1, z + 1)
    def _(dist):
        src = 2 * (z - dist) + c

        @pl.when(has_up)
        def _():
            for d in copies(held(src), src, 0, dist, above):
                d.wait_send()

        for d in copies(held(src), src, 1, dist, other):
            d.wait_send()


def attend(q_t, k_rows, v_t, gates, gain):
    feats, tok = q_t.shape
    heads = feats // HD
    count = lax.axis_size("ep")
    vm = pl.BlockSpec(memory_space=pltpu.VMEM)
    scores = heads * count * tok * tok
    return pl.pallas_call(
        functools.partial(attend_kernel, heads, count),
        out_shape=jax.ShapeDtypeStruct((feats, tok), BF),
        in_specs=[vm] * 5,
        out_specs=vm,
        scratch_shapes=[
            pltpu.VMEM((count,) + k_rows.shape, BF),
            pltpu.VMEM((count,) + v_t.shape, BF),
            pltpu.VMEM((count,) + gates.shape, F32),
            pltpu.VMEM((heads, 2 * LANES, tok), BF),
            pltpu.VMEM((heads, 1, tok), F32),
            pltpu.VMEM((heads, 1, tok), F32),
            pltpu.VMEM((heads, HD, tok), F32),
            pltpu.SemaphoreType.DMA((3, 2, count // 2)),
            pltpu.SemaphoreType.DMA((3, count)),
        ],
        compiler_params=pltpu.CompilerParams(
            vmem_limit_bytes=48 * 1024 * 1024, collective_id=1, has_side_effects=True
        ),
        cost_estimate=pl.CostEstimate(flops=scores * 512, bytes_accessed=2**23, transcendentals=scores),
    )(q_t, k_rows, v_t, gates, gain)


def body(
    attn_in,
    mix_gain,
    query_weight,
    key_weight,
    value_weight,
    query_gain,
    key_gain,
    log_cache,
    head_gain,
    out_weight,
    moe_in,
    moe_gain,
    routes,
    route_weight,
    expert_gate,
    expert_up,
    expert_down,
):
    tok_rows = attn_in.shape[0]
    feats = query_weight.shape[1]
    local_heads = feats // HD
    normed = row_norm(attn_in, mix_gain).astype(BF)

    def project(weight):
        return lax.dot_general(weight, normed, (((0,), (1,)), ((), ())), preferred_element_type=F32)

    def head_norm(x, gain):
        x = x.reshape(local_heads, HD, tok_rows)
        x = x * lax.rsqrt(jnp.mean(x * x, axis=1, keepdims=True) + epsilon)
        return (x * gain[None, :, None]).astype(BF).reshape(feats, tok_rows)

    k_rows = jnp.transpose(head_norm(project(key_weight), key_gain))
    if feats % LANES:
        k_rows = jnp.pad(k_rows, ((0, 0), (0, LANES - feats % LANES)))
    v_t = project(value_weight).astype(BF)
    q_t = head_norm(project(query_weight), query_gain) * jnp.asarray(HD ** -0.5, BF)
    gates = jnp.pad(jnp.transpose(log_cache), ((0, -local_heads % 8), (0, 0)))
    head_t = attend(q_t, k_rows, v_t, gates, head_gain[:, None])
    mixer_out = lax.dot_general(
        lax.all_gather(head_t, "tp", axis=0, tiled=True),
        out_weight,
        (((0,), (0,)), ((), ())),
        preferred_element_type=F32,
    ).astype(BF)

    moe_rows = moe_in.shape[0]
    top_count = routes.shape[1]
    local_experts = expert_gate.shape[0]
    senders = lax.axis_size("ep")
    expert_count = local_experts * senders
    capacity = 3 * moe_rows * top_count // (2 * expert_count)
    model_width = moe_in.shape[1]
    moe_normed = row_norm(moe_in, moe_gain).astype(BF)
    flat_routes = routes.reshape(-1)
    one_hot = (flat_routes[:, None] == jnp.arange(expert_count, dtype=jnp.int32)[None, :]).astype(
        jnp.int32
    )
    order_in = jnp.sum(jnp.cumsum(one_hot, axis=0) * one_hot, axis=1) - 1
    slot_index = flat_routes * capacity + order_in
    slots = jnp.arange(expert_count * capacity, dtype=jnp.int32)
    hit = (slots[:, None, None] == slot_index.reshape(1, moe_rows, top_count)).any(axis=2)
    share_width = model_width // lax.axis_size("tp")
    my_share = lax.dynamic_slice_in_dim(moe_normed, lax.axis_index("tp") * share_width, share_width, 1)
    share_part = (
        jnp.dot(hit.astype(BF), my_share, preferred_element_type=F32)
        .astype(BF)
        .reshape(expert_count, capacity, share_width)
    )
    arrived = lax.all_to_all(share_part, "ep", split_axis=0, concat_axis=0, tiled=True)
    piece_now = lax.all_gather(arrived, "tp", axis=2, tiled=True)
    piece_cols = piece_now.shape[2]
    piece_rows = piece_now.reshape(senders, local_experts, capacity, piece_cols)
    gate_next = jnp.einsum("sjcd,jdf->sjcf", piece_rows, expert_gate, preferred_element_type=F32)
    up_next = jnp.einsum("sjcd,jdf->sjcf", piece_rows, expert_up, preferred_element_type=F32)
    hidden = (jax.nn.silu(gate_next) * up_next).astype(BF)
    partial_value = jnp.einsum("sjcf,jfd->sjcd", hidden, expert_down, preferred_element_type=F32)
    summed = lax.psum_scatter(partial_value.astype(BF), "tp", scatter_dimension=3, tiled=True)
    out_cols = summed.shape[3]
    returned = lax.all_to_all(
        summed.reshape(expert_count, capacity, out_cols),
        "ep",
        split_axis=0,
        concat_axis=0,
        tiled=True,
    )
    flat = returned.reshape(expert_count * capacity, out_cols)
    pick = (slot_index[:, None] == slots[None, :]).astype(BF)
    picked = jnp.dot(pick, flat, preferred_element_type=F32)
    weighted_rows = picked * route_weight.reshape(-1)[:, None]
    moe_out = jnp.sum(weighted_rows.reshape(moe_rows, top_count, out_cols), axis=1).astype(BF)
    return (mixer_out, moe_out)


def solution(mesh):
    in_specs = (
        P("ep", None),
        P(),
        P(None, "tp"),
        P(None, "tp"),
        P(None, "tp"),
        P(),
        P(),
        P("ep", "tp"),
        P("tp"),
        P(None, "tp"),
        P("ep", None),
        P(),
        P("ep", None),
        P("ep", None),
        P("ep", None, "tp"),
        P("ep", None, "tp"),
        P("ep", "tp", None),
    )
    out_specs = (P("ep", "tp"), P("ep", "tp"))
    return jax.shard_map(body, mesh=mesh, in_specs=in_specs, out_specs=out_specs, check_vma=False)
```

```python
import functools

import jax
import jax.numpy as jnp
from jax import lax
from jax.experimental import pallas as pl
from jax.experimental.pallas import tpu as pltpu
from jax.sharding import PartitionSpec as P

HD = 64
LANES = 128
epsilon = 1e-06
BF = jnp.bfloat16
F32 = jnp.float32


def row_norm(inputs, gain_vec):
    floats = inputs.astype(F32)
    scaled = floats * lax.rsqrt(jnp.mean(floats * floats, axis=-1, keepdims=True) + epsilon)
    return scaled * gain_vec


def attend_kernel(
    heads, count, q_ref, k_ref, v_ref, g_ref, gain_ref, o_ref,
    k_all, v_all, g_all, qz, m_s, l_s, acc, send_sem, recv_sem,
):
    me = lax.axis_index("ep")
    chips = count // 2
    z = me // 2
    c = me % 2
    other = 2 * z + 1 - c
    above = 2 * lax.rem(z + 1, chips) + c
    below = 2 * lax.rem(z + chips - 1, chips) + c
    tok = q_ref.shape[1]
    rows8 = g_ref.shape[0]
    own = (k_ref, v_ref, g_ref)
    slots = (k_all, v_all, g_all)

    barrier = pltpu.get_barrier_semaphore()
    for peer in (other, above, below):
        pl.semaphore_signal(barrier, inc=1, device_id={"ep": peer}, device_id_type=pl.DeviceIdType.MESH)
    pl.semaphore_wait(barrier, 3)

    def copies(refs, src, way, dist, target):
        return [
            pltpu.make_async_remote_copy(
                src_ref=refs[i],
                dst_ref=slots[i].at[src],
                send_sem=send_sem.at[i, way, dist],
                recv_sem=recv_sem.at[i, src],
                device_id={"ep": target},
                device_id_type=pl.DeviceIdType.MESH,
            )
            for i in range(3)
        ]

    def held(src):
        return [s.at[src] for s in slots]

    has_up = z + 1 < chips

    @pl.when(has_up)
    def _():
        for d in copies(own, me, 0, 0, above):
            d.start()

    @pl.when(c == 0)
    def _():
        for d in copies(own, me, 1, 0, other):
            d.start()

    row = lax.broadcasted_iota(jnp.int32, (LANES, tok), 0)
    zeros = jnp.zeros((HD, tok), BF)
    for h in range(heads):
        q_h = q_ref[h * HD:(h + 1) * HD, :]
        parts = [q_h, zeros] if h % 2 == 0 else [zeros, q_h]
        hit = (row == h) | (row == rows8 + h) | (row == 2 * rows8 + h)
        pick = jnp.where(hit, -1.0, 0.0).astype(BF)
        qz[h] = jnp.concatenate(parts + [pick], axis=0)

    def step(k_blk, v_blk, g_blk, first=False):
        g = g_blk[...]
        hi = g.astype(BF).astype(F32)
        rest = g - hi
        mid = rest.astype(BF).astype(F32)
        pad = jnp.zeros((LANES - 3 * rows8, tok), F32)
        aug = jnp.concatenate([hi, mid, rest - mid, pad], axis=0).T.astype(BF)
        for h in range(heads):
            p = h // 2
            keys = jnp.concatenate([k_blk[:, p * LANES:(p + 1) * LANES], aug], axis=1)
            s = jnp.dot(keys, qz[h], preferred_element_type=F32)
            if first:
                kpos = lax.broadcasted_iota(jnp.int32, s.shape, 0)
                qpos = lax.broadcasted_iota(jnp.int32, s.shape, 1)
                s = jnp.where(kpos <= qpos, s, -1e30)
            top = jnp.max(s, axis=0, keepdims=True)
            new = top if first else jnp.maximum(m_s[h], top)
            e = jnp.exp(s - new)
            total = jnp.sum(e, axis=0, keepdims=True)
            o = jnp.dot(v_blk[h * HD:(h + 1) * HD, :], e.astype(BF), preferred_element_type=F32)
            if first:
                l_s[h] = total
                acc[h] = o
            else:
                fix = jnp.exp(m_s[h] - new)
                l_s[h] = l_s[h] * fix + total
                acc[h] = acc[h] * fix + o
            m_s[h] = new

    step(*own, first=True)

    def take(src):
        for d in copies(held(src), src, 0, 0, other):
            d.wait_recv()

    @pl.when(c == 1)
    def _():
        take(other)
        step(*held(other))

    @pl.loop(1, z + 1)
    def _(dist):
        src = 2 * (z - dist) + c
        take(src)

        @pl.when(has_up)
        def _():
            for d in copies(held(src), src, 0, dist, above):
                d.start()

        for d in copies(held(src), src, 1, dist, other):
            d.start()
        step(*held(src))
        src2 = 2 * (z - dist) + 1 - c
        take(src2)
        step(*held(src2))

    outs = []
    for h in range(heads):
        a = acc[h] / l_s[h]
        a = a * lax.rsqrt(jnp.mean(a * a, axis=0, keepdims=True) + epsilon)
        outs.append(a * gain_ref[h * HD:(h + 1) * HD, :])
    if heads * HD % LANES:
        outs.append(jnp.zeros((LANES - heads * HD % LANES, tok), F32))
    o_ref[...] = jnp.concatenate(outs, axis=0).T.astype(BF)

    @pl.when(has_up)
    def _():
        for d in copies(own, me, 0, 0, above):
            d.wait_send()

    @pl.when(c == 0)
    def _():
        for d in copies(own, me, 1, 0, other):
            d.wait_send()

    @pl.loop(1, z + 1)
    def _(dist):
        src = 2 * (z - dist) + c

        @pl.when(has_up)
        def _():
            for d in copies(held(src), src, 0, dist, above):
                d.wait_send()

        for d in copies(held(src), src, 1, dist, other):
            d.wait_send()


def attend(q_t, k_rows, v_t, gates, gain):
    feats, tok = q_t.shape
    heads = feats // HD
    count = lax.axis_size("ep")
    vm = pl.BlockSpec(memory_space=pltpu.VMEM)
    scores = heads * count * tok * tok
    return pl.pallas_call(
        functools.partial(attend_kernel, heads, count),
        out_shape=jax.ShapeDtypeStruct((tok, feats + -feats % LANES), BF),
        in_specs=[vm] * 5,
        out_specs=vm,
        scratch_shapes=[
            pltpu.VMEM((count,) + k_rows.shape, BF),
            pltpu.VMEM((count,) + v_t.shape, BF),
            pltpu.VMEM((count,) + gates.shape, F32),
            pltpu.VMEM((heads, 2 * LANES, tok), BF),
            pltpu.VMEM((heads, 1, tok), F32),
            pltpu.VMEM((heads, 1, tok), F32),
            pltpu.VMEM((heads, HD, tok), F32),
            pltpu.SemaphoreType.DMA((3, 2, count // 2)),
            pltpu.SemaphoreType.DMA((3, count)),
        ],
        compiler_params=pltpu.CompilerParams(
            vmem_limit_bytes=48 * 1024 * 1024, collective_id=1, has_side_effects=True
        ),
        cost_estimate=pl.CostEstimate(flops=scores * 512, bytes_accessed=2**23, transcendentals=scores),
    )(q_t, k_rows, v_t, gates, gain)


def tail_kernel(
    ep_count, tp_count, feats, head_ref, w_ref, back_ref, o_ref, ret_ref,
    heads_in, rows_in, total, ep_send, ep_recv, tp_send, tp_recv,
):
    ep = lax.axis_index("ep")
    tp = lax.axis_index("tp")
    mesh_ids = pl.DeviceIdType.MESH
    barrier = pltpu.get_barrier_semaphore()
    for d in range(1, tp_count):
        pl.semaphore_signal(barrier, inc=1, device_id={"tp": lax.rem(tp + d, tp_count)}, device_id_type=mesh_ids)
    for d in range(1, ep_count):
        pl.semaphore_signal(barrier, inc=1, device_id={"ep": lax.rem(ep + d, ep_count)}, device_id_type=mesh_ids)
    pl.semaphore_wait(barrier, ep_count + tp_count - 2)

    def head_copy(d):
        return pltpu.make_async_remote_copy(
            src_ref=head_ref,
            dst_ref=heads_in.at[d],
            send_sem=tp_send.at[d],
            recv_sem=tp_recv.at[d],
            device_id={"tp": lax.rem(tp + d, tp_count)},
            device_id_type=mesh_ids,
        )

    def row_copy(d):
        peer = lax.rem(ep + d, ep_count)
        return pltpu.make_async_remote_copy(
            src_ref=back_ref.at[peer],
            dst_ref=rows_in.at[d],
            send_sem=ep_send.at[d],
            recv_sem=ep_recv.at[d],
            device_id={"ep": peer},
            device_id_type=mesh_ids,
        )

    for d in range(1, tp_count):
        head_copy(d).start()
    for d in range(1, ep_count):
        row_copy(d).start()

    def part(block, owner):
        w = w_ref[pl.ds(pl.multiple_of(owner * feats, feats), feats), :]
        return jnp.dot(block[:, :feats], w, preferred_element_type=F32)

    total[...] = part(head_ref[...], tp)
    ret_ref[ep] = back_ref[ep]
    for d in range(1, tp_count):
        head_copy(d).wait_recv()
        total[...] += part(heads_in[d], lax.rem(tp + tp_count - d, tp_count))
    o_ref[...] = total[...].astype(BF)
    for d in range(1, ep_count):
        row_copy(d).wait_recv()
        ret_ref[lax.rem(ep + ep_count - d, ep_count)] = rows_in[d]
    for d in range(1, tp_count):
        head_copy(d).wait_send()
    for d in range(1, ep_count):
        row_copy(d).wait_send()


def tail(head, weight, back):
    ep_count = lax.axis_size("ep")
    tp_count = lax.axis_size("tp")
    feats = weight.shape[0] // tp_count
    vm = pl.BlockSpec(memory_space=pltpu.VMEM)
    out = (head.shape[0], weight.shape[1])
    return pl.pallas_call(
        functools.partial(tail_kernel, ep_count, tp_count, feats),
        out_shape=(jax.ShapeDtypeStruct(out, BF), jax.ShapeDtypeStruct(back.shape, BF)),
        in_specs=[vm] * 3,
        out_specs=(vm, vm),
        scratch_shapes=[
            pltpu.VMEM((tp_count,) + head.shape, BF),
            pltpu.VMEM(back.shape, BF),
            pltpu.VMEM(out, F32),
            pltpu.SemaphoreType.DMA((ep_count,)),
            pltpu.SemaphoreType.DMA((ep_count,)),
            pltpu.SemaphoreType.DMA((tp_count,)),
            pltpu.SemaphoreType.DMA((tp_count,)),
        ],
        compiler_params=pltpu.CompilerParams(
            vmem_limit_bytes=32 * 1024 * 1024, collective_id=2, has_side_effects=True
        ),
        cost_estimate=pl.CostEstimate(flops=2**30, bytes_accessed=2**22, transcendentals=0),
    )(head, weight, back)


def body(
    attn_in,
    mix_gain,
    query_weight,
    key_weight,
    value_weight,
    query_gain,
    key_gain,
    log_cache,
    head_gain,
    out_weight,
    moe_in,
    moe_gain,
    routes,
    route_weight,
    expert_gate,
    expert_up,
    expert_down,
):
    tok_rows = attn_in.shape[0]
    feats = query_weight.shape[1]
    local_heads = feats // HD
    normed = row_norm(attn_in, mix_gain).astype(BF)

    def project(weight):
        return lax.dot_general(weight, normed, (((0,), (1,)), ((), ())), preferred_element_type=F32)

    def head_norm(x, gain):
        x = x.reshape(local_heads, HD, tok_rows)
        x = x * lax.rsqrt(jnp.mean(x * x, axis=1, keepdims=True) + epsilon)
        return (x * gain[None, :, None]).astype(BF).reshape(feats, tok_rows)

    k_rows = jnp.transpose(head_norm(project(key_weight), key_gain))
    if feats % LANES:
        k_rows = jnp.pad(k_rows, ((0, 0), (0, LANES - feats % LANES)))
    v_t = project(value_weight).astype(BF)
    q_t = head_norm(project(query_weight), query_gain) * jnp.asarray(HD ** -0.5, BF)
    gates = jnp.pad(jnp.transpose(log_cache), ((0, -local_heads % 8), (0, 0)))
    moe_rows = moe_in.shape[0]
    top_count = routes.shape[1]
    local_experts = expert_gate.shape[0]
    senders = lax.axis_size("ep")
    expert_count = local_experts * senders
    capacity = 3 * moe_rows * top_count // (2 * expert_count)
    model_width = moe_in.shape[1]
    moe_normed = row_norm(moe_in, moe_gain).astype(BF)
    flat_routes = routes.reshape(-1)
    one_hot = (flat_routes[:, None] == jnp.arange(expert_count, dtype=jnp.int32)[None, :]).astype(
        jnp.int32
    )
    order_in = jnp.sum(jnp.cumsum(one_hot, axis=0) * one_hot, axis=1) - 1
    slot_index = flat_routes * capacity + order_in
    slots = jnp.arange(expert_count * capacity, dtype=jnp.int32)
    hit = (slots[:, None, None] == slot_index.reshape(1, moe_rows, top_count)).any(axis=2)
    share_width = model_width // lax.axis_size("tp")
    my_share = lax.dynamic_slice_in_dim(moe_normed, lax.axis_index("tp") * share_width, share_width, 1)
    share_part = (
        jnp.dot(hit.astype(BF), my_share, preferred_element_type=F32)
        .astype(BF)
        .reshape(expert_count, capacity, share_width)
    )
    arrived = lax.all_to_all(share_part, "ep", split_axis=0, concat_axis=0, tiled=True)
    piece_now = lax.all_gather(arrived, "tp", axis=2, tiled=True)
    piece_now, q_t, k_rows, v_t = lax.optimization_barrier((piece_now, q_t, k_rows, v_t))
    piece_cols = piece_now.shape[2]
    piece_rows = piece_now.reshape(senders, local_experts, capacity, piece_cols)
    gate_next = jnp.einsum("sjcd,jdf->sjcf", piece_rows, expert_gate, preferred_element_type=F32)
    up_next = jnp.einsum("sjcd,jdf->sjcf", piece_rows, expert_up, preferred_element_type=F32)
    hidden = (jax.nn.silu(gate_next) * up_next).astype(BF)
    partial_value = jnp.einsum("sjcf,jfd->sjcd", hidden, expert_down, preferred_element_type=F32)
    partial_value, q_t = lax.optimization_barrier((partial_value.astype(BF), q_t))
    summed = lax.psum_scatter(partial_value, "tp", scatter_dimension=3, tiled=True)
    out_cols = summed.shape[3]
    head = attend(q_t, k_rows, v_t, gates, head_gain[:, None])
    mixer_out, returned = tail(head, out_weight, summed.reshape(expert_count, capacity, out_cols))
    flat = returned.reshape(expert_count * capacity, out_cols)
    pick = (slot_index[:, None] == slots[None, :]).astype(BF)
    picked = jnp.dot(pick, flat, preferred_element_type=F32)
    weighted_rows = picked * route_weight.reshape(-1)[:, None]
    moe_out = jnp.sum(weighted_rows.reshape(moe_rows, top_count, out_cols), axis=1).astype(BF)
    return (mixer_out, moe_out)


def solution(mesh):
    in_specs = (
        P("ep", None),
        P(),
        P(None, "tp"),
        P(None, "tp"),
        P(None, "tp"),
        P(),
        P(),
        P("ep", "tp"),
        P("tp"),
        P(None, "tp"),
        P("ep", None),
        P(),
        P("ep", None),
        P("ep", None),
        P("ep", None, "tp"),
        P("ep", None, "tp"),
        P("ep", "tp", None),
    )
    out_specs = (P("ep", "tp"), P("ep", "tp"))
    return jax.shard_map(body, mesh=mesh, in_specs=in_specs, out_specs=out_specs, check_vma=False)
```

```python
import functools

import jax
import jax.numpy as jnp
from jax import lax
from jax.experimental import pallas as pl
from jax.experimental.pallas import tpu as pltpu
from jax.sharding import PartitionSpec as P

HD = 64
LANES = 128
epsilon = 1e-06
BF = jnp.bfloat16
F32 = jnp.float32


def row_norm(inputs, gain_vec):
    floats = inputs.astype(F32)
    scaled = floats * lax.rsqrt(jnp.mean(floats * floats, axis=-1, keepdims=True) + epsilon)
    return scaled * gain_vec


def attend_kernel(
    heads, count, q_ref, k_ref, v_ref, g_ref, gain_ref, o_ref,
    k_all, v_all, g_all, qz, m_s, l_s, acc, send_sem, recv_sem,
):
    me = lax.axis_index("ep")
    chips = count // 2
    z = me // 2
    c = me % 2
    other = 2 * z + 1 - c
    above = 2 * lax.rem(z + 1, chips) + c
    below = 2 * lax.rem(z + chips - 1, chips) + c
    tok = q_ref.shape[1]
    rows8 = g_ref.shape[0]
    own = (k_ref, v_ref, g_ref)
    slots = (k_all, v_all, g_all)

    barrier = pltpu.get_barrier_semaphore()
    for peer in (other, above, below):
        pl.semaphore_signal(barrier, inc=1, device_id={"ep": peer}, device_id_type=pl.DeviceIdType.MESH)
    pl.semaphore_wait(barrier, 3)

    def copies(refs, src, way, dist, target):
        return [
            pltpu.make_async_remote_copy(
                src_ref=refs[i],
                dst_ref=slots[i].at[src],
                send_sem=send_sem.at[i, way, dist],
                recv_sem=recv_sem.at[i, src],
                device_id={"ep": target},
                device_id_type=pl.DeviceIdType.MESH,
            )
            for i in range(3)
        ]

    def held(src):
        return [s.at[src] for s in slots]

    has_up = z + 1 < chips

    @pl.when(has_up)
    def _():
        for d in copies(own, me, 0, 0, above):
            d.start()

    @pl.when(c == 0)
    def _():
        for d in copies(own, me, 1, 0, other):
            d.start()

    row = lax.broadcasted_iota(jnp.int32, (LANES, tok), 0)
    zeros = jnp.zeros((HD, tok), BF)
    for h in range(heads):
        q_h = q_ref[h * HD:(h + 1) * HD, :]
        parts = [q_h, zeros] if h % 2 == 0 else [zeros, q_h]
        hit = (row == h) | (row == rows8 + h) | (row == 2 * rows8 + h)
        pick = jnp.where(hit, -1.0, 0.0).astype(BF)
        qz[h] = jnp.concatenate(parts + [pick], axis=0)

    def step(k_blk, v_blk, g_blk, first=False):
        g = g_blk[...]
        hi = g.astype(BF).astype(F32)
        rest = g - hi
        mid = rest.astype(BF).astype(F32)
        pad = jnp.zeros((LANES - 3 * rows8, tok), F32)
        aug = jnp.concatenate([hi, mid, rest - mid, pad], axis=0).T.astype(BF)
        for h in range(heads):
            p = h // 2
            keys = jnp.concatenate([k_blk[:, p * LANES:(p + 1) * LANES], aug], axis=1)
            s = jnp.dot(keys, qz[h], preferred_element_type=F32)
            if first:
                kpos = lax.broadcasted_iota(jnp.int32, s.shape, 0)
                qpos = lax.broadcasted_iota(jnp.int32, s.shape, 1)
                s = jnp.where(kpos <= qpos, s, -1e30)
            top = jnp.max(s, axis=0, keepdims=True)
            new = top if first else jnp.maximum(m_s[h], top)
            e = jnp.exp(s - new)
            total = jnp.sum(e, axis=0, keepdims=True)
            o = jnp.dot(v_blk[h * HD:(h + 1) * HD, :], e.astype(BF), preferred_element_type=F32)
            if first:
                l_s[h] = total
                acc[h] = o
            else:
                fix = jnp.exp(m_s[h] - new)
                l_s[h] = l_s[h] * fix + total
                acc[h] = acc[h] * fix + o
            m_s[h] = new

    step(*own, first=True)

    def take(src):
        for d in copies(held(src), src, 0, 0, other):
            d.wait_recv()

    @pl.when(c == 1)
    def _():
        take(other)
        step(*held(other))

    @pl.loop(1, z + 1)
    def _(dist):
        src = 2 * (z - dist) + c
        take(src)

        @pl.when(has_up)
        def _():
            for d in copies(held(src), src, 0, dist, above):
                d.start()

        for d in copies(held(src), src, 1, dist, other):
            d.start()
        step(*held(src))
        src2 = 2 * (z - dist) + 1 - c
        take(src2)
        step(*held(src2))

    outs = []
    for h in range(heads):
        a = acc[h] / l_s[h]
        a = a * lax.rsqrt(jnp.mean(a * a, axis=0, keepdims=True) + epsilon)
        outs.append(a * gain_ref[h * HD:(h + 1) * HD, :])
    if heads * HD % LANES:
        outs.append(jnp.zeros((LANES - heads * HD % LANES, tok), F32))
    o_ref[...] = jnp.concatenate(outs, axis=0).T.astype(BF)

    @pl.when(has_up)
    def _():
        for d in copies(own, me, 0, 0, above):
            d.wait_send()

    @pl.when(c == 0)
    def _():
        for d in copies(own, me, 1, 0, other):
            d.wait_send()

    @pl.loop(1, z + 1)
    def _(dist):
        src = 2 * (z - dist) + c

        @pl.when(has_up)
        def _():
            for d in copies(held(src), src, 0, dist, above):
                d.wait_send()

        for d in copies(held(src), src, 1, dist, other):
            d.wait_send()


def attend(q_t, k_rows, v_t, gates, gain):
    feats, tok = q_t.shape
    heads = feats // HD
    count = lax.axis_size("ep")
    vm = pl.BlockSpec(memory_space=pltpu.VMEM)
    scores = heads * count * tok * tok
    return pl.pallas_call(
        functools.partial(attend_kernel, heads, count),
        out_shape=jax.ShapeDtypeStruct((tok, feats + -feats % LANES), BF),
        in_specs=[vm] * 5,
        out_specs=vm,
        scratch_shapes=[
            pltpu.VMEM((count,) + k_rows.shape, BF),
            pltpu.VMEM((count,) + v_t.shape, BF),
            pltpu.VMEM((count,) + gates.shape, F32),
            pltpu.VMEM((heads, 2 * LANES, tok), BF),
            pltpu.VMEM((heads, 1, tok), F32),
            pltpu.VMEM((heads, 1, tok), F32),
            pltpu.VMEM((heads, HD, tok), F32),
            pltpu.SemaphoreType.DMA((3, 2, count // 2)),
            pltpu.SemaphoreType.DMA((3, count)),
        ],
        compiler_params=pltpu.CompilerParams(
            vmem_limit_bytes=48 * 1024 * 1024, collective_id=1, has_side_effects=True
        ),
        cost_estimate=pl.CostEstimate(flops=scores * 512, bytes_accessed=2**23, transcendentals=scores),
    )(q_t, k_rows, v_t, gates, gain)


def tail_kernel(
    ep_count, tp_count, feats, head_ref, w_ref, back_ref, o_ref, ret_ref,
    heads_in, rows_in, total, ep_send, ep_recv, tp_send, tp_recv,
):
    ep = lax.axis_index("ep")
    tp = lax.axis_index("tp")
    mesh_ids = pl.DeviceIdType.MESH
    barrier = pltpu.get_barrier_semaphore()
    for d in range(1, tp_count):
        pl.semaphore_signal(barrier, inc=1, device_id={"tp": lax.rem(tp + d, tp_count)}, device_id_type=mesh_ids)
    for d in range(1, ep_count):
        pl.semaphore_signal(barrier, inc=1, device_id={"ep": lax.rem(ep + d, ep_count)}, device_id_type=mesh_ids)
    pl.semaphore_wait(barrier, ep_count + tp_count - 2)

    def head_copy(d):
        return pltpu.make_async_remote_copy(
            src_ref=head_ref,
            dst_ref=heads_in.at[d],
            send_sem=tp_send.at[d],
            recv_sem=tp_recv.at[d],
            device_id={"tp": lax.rem(tp + d, tp_count)},
            device_id_type=mesh_ids,
        )

    def row_copy(d):
        peer = lax.rem(ep + d, ep_count)
        return pltpu.make_async_remote_copy(
            src_ref=back_ref.at[peer],
            dst_ref=rows_in.at[d],
            send_sem=ep_send.at[d],
            recv_sem=ep_recv.at[d],
            device_id={"ep": peer},
            device_id_type=mesh_ids,
        )

    for d in range(1, tp_count):
        head_copy(d).start()
    for d in range(1, ep_count):
        row_copy(d).start()

    def part(block, owner):
        w = w_ref[pl.ds(pl.multiple_of(owner * feats, feats), feats), :]
        return jnp.dot(block[:, :feats], w, preferred_element_type=F32)

    total[...] = part(head_ref[...], tp)
    ret_ref[ep] = back_ref[ep]
    for d in range(1, tp_count):
        head_copy(d).wait_recv()
        total[...] += part(heads_in[d], lax.rem(tp + tp_count - d, tp_count))
    o_ref[...] = total[...].astype(BF)
    for d in range(1, ep_count):
        row_copy(d).wait_recv()
        ret_ref[lax.rem(ep + ep_count - d, ep_count)] = rows_in[d]
    for d in range(1, tp_count):
        head_copy(d).wait_send()
    for d in range(1, ep_count):
        row_copy(d).wait_send()


def tail(head, weight, back):
    ep_count = lax.axis_size("ep")
    tp_count = lax.axis_size("tp")
    feats = weight.shape[0] // tp_count
    vm = pl.BlockSpec(memory_space=pltpu.VMEM)
    out = (head.shape[0], weight.shape[1])
    return pl.pallas_call(
        functools.partial(tail_kernel, ep_count, tp_count, feats),
        out_shape=(jax.ShapeDtypeStruct(out, BF), jax.ShapeDtypeStruct(back.shape, BF)),
        in_specs=[vm] * 3,
        out_specs=(vm, vm),
        scratch_shapes=[
            pltpu.VMEM((tp_count,) + head.shape, BF),
            pltpu.VMEM(back.shape, BF),
            pltpu.VMEM(out, F32),
            pltpu.SemaphoreType.DMA((ep_count,)),
            pltpu.SemaphoreType.DMA((ep_count,)),
            pltpu.SemaphoreType.DMA((tp_count,)),
            pltpu.SemaphoreType.DMA((tp_count,)),
        ],
        compiler_params=pltpu.CompilerParams(
            vmem_limit_bytes=32 * 1024 * 1024, collective_id=2, has_side_effects=True
        ),
        cost_estimate=pl.CostEstimate(flops=2**30, bytes_accessed=2**22, transcendentals=0),
    )(head, weight, back)


def swap_kernel(count, src_ref, o_ref, rows_in, send_sem, recv_sem):
    ep = lax.axis_index("ep")
    mesh_ids = pl.DeviceIdType.MESH
    barrier = pltpu.get_barrier_semaphore()
    for d in range(1, count):
        pl.semaphore_signal(barrier, inc=1, device_id={"ep": lax.rem(ep + d, count)}, device_id_type=mesh_ids)
    pl.semaphore_wait(barrier, count - 1)

    def row_copy(d):
        peer = lax.rem(ep + d, count)
        return pltpu.make_async_remote_copy(
            src_ref=src_ref.at[peer],
            dst_ref=rows_in.at[d],
            send_sem=send_sem.at[d],
            recv_sem=recv_sem.at[d],
            device_id={"ep": peer},
            device_id_type=mesh_ids,
        )

    for d in range(1, count):
        row_copy(d).start()
    o_ref[ep] = src_ref[ep]
    for d in range(1, count):
        row_copy(d).wait_recv()
        o_ref[lax.rem(ep + count - d, count)] = rows_in[d]
    for d in range(1, count):
        row_copy(d).wait_send()


def swap(blocks):
    count = lax.axis_size("ep")
    vm = pl.BlockSpec(memory_space=pltpu.VMEM)
    return pl.pallas_call(
        functools.partial(swap_kernel, count),
        out_shape=jax.ShapeDtypeStruct(blocks.shape, BF),
        in_specs=[vm],
        out_specs=vm,
        scratch_shapes=[
            pltpu.VMEM(blocks.shape, BF),
            pltpu.SemaphoreType.DMA((count,)),
            pltpu.SemaphoreType.DMA((count,)),
        ],
        compiler_params=pltpu.CompilerParams(
            vmem_limit_bytes=16 * 1024 * 1024, collective_id=3, has_side_effects=True
        ),
        cost_estimate=pl.CostEstimate(flops=2**27, bytes_accessed=2**22, transcendentals=0),
    )(blocks)


def body(
    attn_in,
    mix_gain,
    query_weight,
    key_weight,
    value_weight,
    query_gain,
    key_gain,
    log_cache,
    head_gain,
    out_weight,
    moe_in,
    moe_gain,
    routes,
    route_weight,
    expert_gate,
    expert_up,
    expert_down,
):
    tok_rows = attn_in.shape[0]
    feats = query_weight.shape[1]
    local_heads = feats // HD
    normed = row_norm(attn_in, mix_gain).astype(BF)

    def project(weight):
        return lax.dot_general(weight, normed, (((0,), (1,)), ((), ())), preferred_element_type=F32)

    def head_norm(x, gain):
        x = x.reshape(local_heads, HD, tok_rows)
        x = x * lax.rsqrt(jnp.mean(x * x, axis=1, keepdims=True) + epsilon)
        return (x * gain[None, :, None]).astype(BF).reshape(feats, tok_rows)

    k_rows = jnp.transpose(head_norm(project(key_weight), key_gain))
    if feats % LANES:
        k_rows = jnp.pad(k_rows, ((0, 0), (0, LANES - feats % LANES)))
    v_t = project(value_weight).astype(BF)
    q_t = head_norm(project(query_weight), query_gain) * jnp.asarray(HD ** -0.5, BF)
    gates = jnp.pad(jnp.transpose(log_cache), ((0, -local_heads % 8), (0, 0)))
    moe_rows = moe_in.shape[0]
    top_count = routes.shape[1]
    local_experts = expert_gate.shape[0]
    senders = lax.axis_size("ep")
    expert_count = local_experts * senders
    capacity = 3 * moe_rows * top_count // (2 * expert_count)
    model_width = moe_in.shape[1]
    moe_normed = row_norm(moe_in, moe_gain).astype(BF)
    flat_routes = routes.reshape(-1)
    one_hot = (flat_routes[:, None] == jnp.arange(expert_count, dtype=jnp.int32)[None, :]).astype(
        jnp.int32
    )
    order_in = jnp.sum(jnp.cumsum(one_hot, axis=0) * one_hot, axis=1) - 1
    slot_index = flat_routes * capacity + order_in
    slots = jnp.arange(expert_count * capacity, dtype=jnp.int32)
    hit = (slots[:, None, None] == slot_index.reshape(1, moe_rows, top_count)).any(axis=2)
    share_width = model_width // lax.axis_size("tp")
    my_share = lax.dynamic_slice_in_dim(moe_normed, lax.axis_index("tp") * share_width, share_width, 1)
    share_part = (
        jnp.dot(hit.astype(BF), my_share, preferred_element_type=F32)
        .astype(BF)
        .reshape(expert_count, capacity, share_width)
    )
    arrived = swap(share_part)
    piece_now = lax.all_gather(arrived, "tp", axis=2, tiled=True)
    piece_now, q_t, k_rows, v_t = lax.optimization_barrier((piece_now, q_t, k_rows, v_t))
    piece_cols = piece_now.shape[2]
    piece_rows = piece_now.reshape(senders, local_experts, capacity, piece_cols)
    gate_next = jnp.einsum("sjcd,jdf->sjcf", piece_rows, expert_gate, preferred_element_type=F32)
    up_next = jnp.einsum("sjcd,jdf->sjcf", piece_rows, expert_up, preferred_element_type=F32)
    hidden = (jax.nn.silu(gate_next) * up_next).astype(BF)
    partial_value = jnp.einsum("sjcf,jfd->sjcd", hidden, expert_down, preferred_element_type=F32)
    partial_value, q_t = lax.optimization_barrier((partial_value.astype(BF), q_t))
    summed = lax.psum_scatter(partial_value, "tp", scatter_dimension=3, tiled=True)
    out_cols = summed.shape[3]
    head = attend(q_t, k_rows, v_t, gates, head_gain[:, None])
    mixer_out, returned = tail(head, out_weight, summed.reshape(expert_count, capacity, out_cols))
    flat = returned.reshape(expert_count * capacity, out_cols)
    pick = (slot_index[:, None] == slots[None, :]).astype(BF)
    picked = jnp.dot(pick, flat, preferred_element_type=F32)
    weighted_rows = picked * route_weight.reshape(-1)[:, None]
    moe_out = jnp.sum(weighted_rows.reshape(moe_rows, top_count, out_cols), axis=1).astype(BF)
    return (mixer_out, moe_out)


def solution(mesh):
    in_specs = (
        P("ep", None),
        P(),
        P(None, "tp"),
        P(None, "tp"),
        P(None, "tp"),
        P(),
        P(),
        P("ep", "tp"),
        P("tp"),
        P(None, "tp"),
        P("ep", None),
        P(),
        P("ep", None),
        P("ep", None),
        P("ep", None, "tp"),
        P("ep", None, "tp"),
        P("ep", "tp", None),
    )
    out_specs = (P("ep", "tp"), P("ep", "tp"))
    return jax.shard_map(body, mesh=mesh, in_specs=in_specs, out_specs=out_specs, check_vma=False)
```
